512 devices in a mesh: kv: 32 (over z, x), tp: 16 (over y, core).
Axes of the slice: x: 4, y: 8, z: 8, core: 2. Of those that a mesh axis runs over, the one named last changes fastest.
Arguments:
- tokens: bfloat16 [16, 4096], P(None, ('kv', 'tp')), may hold values from -24 to 24
- live_lengths: int32 [16], replicated, may hold values from 256 to 16384, as said below
- kv_cache: bfloat16 [16, 16384, 2048], P(None, 'kv', 'tp'), may hold values from -128 to 128
- gate_sums: float32 [16, 16, 16384], P(None, 'tp', 'kv'), may hold values from -16384 to 0, as said below
- w_query: bfloat16 [4096, 4096], P('kv', 'tp'), may hold values from -0.09375 to 0.09375
- w_key: bfloat16 [4096, 1024], P('kv', 'tp'), may hold values from -0.09375 to 0.09375
- w_value: bfloat16 [4096, 1024], P('kv', 'tp'), may hold values from -0.09375 to 0.09375
- w_forget: bfloat16 [4096, 16], replicated, may hold values from -0.09375 to 0.09375
- forget_bias: float32 [16], replicated, may hold values from -1 to 2
- w_out: bfloat16 [4096, 4096], P('tp', 'kv'), may hold values from -0.75 to 0.75
- first_gain: float32 [4096], P(('kv', 'tp')), may hold values from 0 to 4
- w_gate: bfloat16 [4096, 11264], P('kv', 'tp'), may hold values from -0.09375 to 0.09375
- w_up: bfloat16 [4096, 11264], P('kv', 'tp'), may hold values from -0.09375 to 0.09375
- w_down: bfloat16 [11264, 4096], P('tp', 'kv'), may hold values from -0.109375 to 0.109375
- second_gain: float32 [4096], P(('kv', 'tp')), may hold values from 0 to 4
Outputs:
- layer_out: bfloat16 [16, 4096], P(None, ('kv', 'tp'))
The draws below stay inside these ranges and needn't reach their ends.
Inputs may be any that keep to these rules, and one draw needn't show every extreme that they name: `live_lengths`: at least one sequence has length exactly 16384. `gate_sums`: entries at positions at or beyond the sequence's length are 0.
All inputs are finite; a program needn't handle non-finite values.
Results may differ from the reference program's by a relative error of at most 0.019.
Values may be sent and summed in bfloat16 or wider, within the bound.
A program may use at most 64 MiB of HBM per device.

```python
import jax
import jax.numpy as jnp
from jax import lax

D = 4096
DH = 64
KEY_HEAD_COUNT = 16
GROUP = 4
H = 64
FF = 11264
SEQUENCE_COUNT = 16
P_DEV = 512
LEN = 16384


def sequence_lengths(key):
    base_key = jax.random.fold_in(key, 701)
    short_key, long_key, order_key = jax.random.split(base_key, 3)
    short_floor = max(LEN // 64, 2)
    short_lengths = jax.random.randint(short_key, (SEQUENCE_COUNT,), short_floor, max(LEN // 8, short_floor) + 1)
    long_lengths = jax.random.randint(long_key, (SEQUENCE_COUNT,), max(LEN // 2, 2), LEN + 1)
    ranking = jax.random.permutation(order_key, SEQUENCE_COUNT)
    chosen = jnp.where(ranking < max(SEQUENCE_COUNT // 4, 1), long_lengths, short_lengths)
    return jnp.where(ranking == 0, LEN, chosen).astype(jnp.int32)


def column_scales(key, rise_factor):
    jitter_strength = jax.random.uniform(key, (D,), jnp.float32, 0.8, 1.25)
    where_col = jnp.arange(D, dtype=jnp.float32) / max(D - 1, 1)
    return jitter_strength * jnp.exp(jnp.log(rise_factor) * (where_col - 0.5))


def token_rows(key):
    base_key = jax.random.fold_in(key, 702)
    noise_key, scale_key = jax.random.split(base_key, 2)
    noise_draw = jnp.clip(jax.random.normal(noise_key, (SEQUENCE_COUNT, D), jnp.float32), -6.0, 6.0)
    scales = column_scales(scale_key, 3.0)[None, :]
    return noise_draw * scales + scales


def query_weight(key):
    base_key = jax.random.fold_in(key, 703)
    return jnp.clip(jax.random.normal(base_key, (D, H * DH), jnp.float32), -6.0, 6.0) * D ** (-0.5)


def log_uniform(key, array_shape, lower_end, upper_end):
    return jnp.exp(jax.random.uniform(key, array_shape, jnp.float32, jnp.log(lower_end), jnp.log(upper_end)))


def rising_gain(key, salt_value):
    base_key = jax.random.fold_in(key, salt_value)
    return column_scales(base_key, 3.0)


def draw_tokens(key, part):
    return token_rows(key).astype(jnp.bfloat16)


def draw_live_lengths(key, part):
    return sequence_lengths(key)


def draw_w_query(key, part):
    return query_weight(key).astype(jnp.bfloat16)


def draw_first_gain(key, part):
    return rising_gain(key, 706)


def draw_second_gain(key, part):
    return rising_gain(key, 707)


def draw_kv_cache(key, part):
    base_key = jax.random.fold_in(key, 704)
    noise_key, offset_key = jax.random.split(base_key, 2)
    entries = jnp.clip(jax.random.normal(noise_key, (SEQUENCE_COUNT, LEN, KEY_HEAD_COUNT, 2, DH), jnp.float32), -6.0, 6.0)
    block_count = (LEN + 63) // 64
    offsets = jnp.clip(jax.random.normal(offset_key, (SEQUENCE_COUNT, block_count, 1, KEY_HEAD_COUNT, 1, DH), jnp.float32), -3.0, 3.0)
    offsets = jnp.broadcast_to(offsets, (SEQUENCE_COUNT, block_count, 64, KEY_HEAD_COUNT, 1, DH)).reshape(SEQUENCE_COUNT, block_count * 64, KEY_HEAD_COUNT, 1, DH)[:, :LEN]
    slot_pick = jnp.array([0.0, 1.0], jnp.float32).reshape(1, 1, 1, 2, 1)
    entries = entries + offsets * slot_pick
    return entries.reshape(SEQUENCE_COUNT, LEN, KEY_HEAD_COUNT * 2 * DH).astype(jnp.bfloat16)


def draw_gate_sums(key, part):
    base_key = jax.random.fold_in(key, 705)
    head_key, fast_key, slow_key, block_key, rough_key, location_random_key, depth_key = jax.random.split(base_key, 7)
    length_values = sequence_lengths(key)
    head_order = jax.random.permutation(head_key, KEY_HEAD_COUNT)
    quick_decay_heads = head_order < max(KEY_HEAD_COUNT // 2, 1)
    fast_rate = log_uniform(fast_key, (SEQUENCE_COUNT, KEY_HEAD_COUNT, 1), 0.04, 0.12)
    slow_rate = log_uniform(slow_key, (SEQUENCE_COUNT, KEY_HEAD_COUNT, 1), 0.2, 0.8) / LEN
    increment_ratio = jnp.where(quick_decay_heads[None, :, None], fast_rate, slow_rate)
    block_count = (LEN + P_DEV - 1) // P_DEV
    block_multiplier = log_uniform(block_key, (SEQUENCE_COUNT, KEY_HEAD_COUNT, block_count, 1), 0.5, 2.0)
    block_multiplier = jnp.broadcast_to(block_multiplier, (SEQUENCE_COUNT, KEY_HEAD_COUNT, block_count, P_DEV)).reshape(SEQUENCE_COUNT, KEY_HEAD_COUNT, block_count * P_DEV)[:, :, :LEN]
    jitter_strength = jax.random.uniform(rough_key, (SEQUENCE_COUNT, KEY_HEAD_COUNT, LEN), jnp.float32, 0.5, 1.5)
    spike_locations = jax.random.randint(location_random_key, (SEQUENCE_COUNT, KEY_HEAD_COUNT, 3), 0, length_values[:, None, None])
    depth_values = jnp.log(jax.random.uniform(depth_key, (SEQUENCE_COUNT, KEY_HEAD_COUNT, 3), jnp.float32, 0.5, 0.8))
    position_selector = jnp.arange(LEN, dtype=jnp.int32)
    spike_decrease = jnp.sum(jnp.where(position_selector[None, None, None, :] == spike_locations[..., None], depth_values[..., None], 0.0), axis=2)
    spike_decrease = jnp.where(quick_decay_heads[None, :, None], 0.0, spike_decrease)
    logarithm_gate_values = -increment_ratio * block_multiplier * jitter_strength + spike_decrease
    live_mask = position_selector[None, None, :] < length_values[:, None, None]
    masked = jnp.where(live_mask, logarithm_gate_values, 0.0)
    suffix_sum = jnp.flip(jnp.cumsum(jnp.flip(masked, axis=-1), axis=-1), axis=-1) - masked
    return suffix_sum


def spiked(drawn, own_key, source, target, blocks, factor):
    owner, partner = [(jnp.arange(drawn.shape[axis_at]) // (drawn.shape[axis_at] // blocks)).reshape([-1 if axis == axis_at else 1 for axis in range(drawn.ndim)]) for axis_at in (source, target)]
    chosen = jax.random.permutation(own_key, blocks)[partner]
    strong = (owner == chosen) | (owner == (partner + blocks // 2) % blocks)
    return jnp.where(strong, factor * drawn, drawn)


def block_scale(own_key, extent, shards, least, largest):
    def one(dim, parts):
        steps = jax.random.uniform(jax.random.fold_in(jax.random.fold_in(own_key, 6), dim), (parts,), jnp.float32, least / len(shards), largest / len(shards))
        return jnp.repeat(jnp.exp(steps), extent[dim] // parts).reshape((-1,) + (1,) * (len(extent) - dim - 1))

    loudness = one(*shards[0])
    for cut in shards[1:]:
        loudness = loudness * one(*cut)
    return loudness


def scatter_about(rng, extent, width, bound, cuts=(), kind=jnp.bfloat16):
    level = block_scale(rng, extent, cuts, -0.22, 0.18) if cuts else 1.0
    values = jax.random.normal(rng, extent, jnp.float32) * width * level
    return jnp.minimum(jnp.maximum(values, -bound), bound).astype(kind)


def gaussian_with(own_key, extent, deviation, most, cuts, heavy, kind=jnp.bfloat16):
    drawn = deviation * jax.random.normal(own_key, extent, jnp.float32)
    if cuts:
        drawn = drawn * block_scale(own_key, extent, cuts, -0.22, 0.18)
    return jnp.clip(spiked(drawn, jax.random.fold_in(own_key, 3), *heavy), -most, most).astype(kind)


def setup_inputs(seed: int = 0) -> dict:
    arg_keys = jax.random.split(jax.random.key(seed), 16)
    tokens = draw_tokens(jax.random.fold_in(arg_keys[15], 71), 0)
    live_lengths = draw_live_lengths(jax.random.fold_in(arg_keys[15], 71), 0)
    kv_cache = draw_kv_cache(jax.random.fold_in(arg_keys[15], 71), 0)
    gate_sums = draw_gate_sums(jax.random.fold_in(arg_keys[15], 71), 0)
    w_query = draw_w_query(jax.random.fold_in(arg_keys[15], 71), 0)
    w_key = scatter_about(arg_keys[5], (D, KEY_HEAD_COUNT * DH), D ** -0.5, 0.09375, ((0, 32), (1, 16)))
    w_value = scatter_about(arg_keys[6], (D, KEY_HEAD_COUNT * DH), D ** -0.5, 0.09375, ((0, 32), (1, 16)))
    w_forget = scatter_about(arg_keys[7], (D, KEY_HEAD_COUNT), D ** -0.5, 0.09375)
    forget_bias = jnp.clip(jax.random.uniform(arg_keys[8], (KEY_HEAD_COUNT,), jnp.float32, -1.0, 2.0), -1.0, 2.0)
    w_out = gaussian_with(arg_keys[9], (H * DH, D), (H * DH // 16) ** -0.5, 0.75, ((0, 16), (1, 32)), (0, 1, 32, 2.75))
    first_gain = draw_first_gain(jax.random.fold_in(arg_keys[15], 71), 0)
    w_gate = scatter_about(arg_keys[11], (D, FF), D ** -0.5, 0.09375, ((0, 32), (1, 16)))
    w_up = scatter_about(arg_keys[12], (D, FF), D ** -0.5, 0.09375, ((0, 32), (1, 16)))
    w_down = gaussian_with(arg_keys[13], (FF, D), FF ** -0.5, 0.109375, ((0, 16), (1, 32)), (0, 1, 32, 2.75))
    second_gain = draw_second_gain(jax.random.fold_in(arg_keys[15], 71), 0)
    return {"tokens": tokens, "live_lengths": live_lengths, "kv_cache": kv_cache, "gate_sums": gate_sums, "w_query": w_query, "w_key": w_key, "w_value": w_value, "w_forget": w_forget, "forget_bias": forget_bias, "w_out": w_out, "first_gain": first_gain, "w_gate": w_gate, "w_up": w_up, "w_down": w_down, "second_gain": second_gain}


EPSILON = 1e-05

def layer_norm(mixture, norm_gain):
    centre = lax.optimization_barrier(jnp.mean(mixture, axis=-1, keepdims=True))
    spread = lax.optimization_barrier(jnp.mean(jnp.square(mixture - centre), axis=-1, keepdims=True))
    return ((mixture - centre) * lax.rsqrt(spread + EPSILON) * norm_gain).astype(jnp.bfloat16)

def attend_sequence(pieces):
    query_row, new_key, new_value, new_gate, cache_rows, gate_row, length = pieces
    queries = query_row.astype(jnp.float32).reshape(KEY_HEAD_COUNT, GROUP, DH)
    blocks = cache_rows.astype(jnp.float32).reshape(LEN, KEY_HEAD_COUNT, 2, DH)
    score_scale = DH ** (-0.5)
    scores = jnp.einsum('gjd,sgd->gjs', queries, blocks[:, :, 0, :]) * score_scale
    scores = scores + gate_row[:, None, :] + new_gate[:, None, None]
    live_mask = jnp.arange(LEN, dtype=jnp.int32) < length
    own_score = jnp.einsum('gjd,gd->gj', queries, new_key.astype(jnp.float32).reshape(KEY_HEAD_COUNT, DH)) * score_scale
    row_top = jnp.maximum(lax.optimization_barrier(jnp.max(jnp.where(live_mask, scores, -jnp.inf), axis=-1)), own_score)
    weights = jnp.where(live_mask, jnp.exp(scores - row_top[..., None]), 0.0)
    own_weight = jnp.exp(own_score - row_top)
    weight_total = lax.optimization_barrier(jnp.sum(weights, axis=-1)) + own_weight
    rounded = lax.optimization_barrier(weights.astype(jnp.bfloat16)).astype(jnp.float32)
    own_rounded = lax.optimization_barrier(own_weight.astype(jnp.bfloat16)).astype(jnp.float32)
    summed = jnp.einsum('gjs,sgd->gjd', rounded, blocks[:, :, 1, :])
    summed = summed + own_rounded[..., None] * new_value.astype(jnp.float32).reshape(KEY_HEAD_COUNT, 1, DH)
    return (summed / weight_total[..., None]).reshape(KEY_HEAD_COUNT * GROUP * DH).astype(jnp.bfloat16)

def reference(tokens, live_lengths, kv_cache, gate_sums, w_query, w_key, w_value, w_forget, forget_bias, w_out, first_gain, w_gate, w_up, w_down, second_gain):
    queries = jnp.dot(tokens, w_query, preferred_element_type=jnp.float32).astype(jnp.bfloat16)
    new_keys = jnp.dot(tokens, w_key, preferred_element_type=jnp.float32).astype(jnp.bfloat16)
    new_values = jnp.dot(tokens, w_value, preferred_element_type=jnp.float32).astype(jnp.bfloat16)
    new_gates = jax.nn.log_sigmoid(jnp.dot(tokens, w_forget, preferred_element_type=jnp.float32) + forget_bias)
    attended = lax.map(attend_sequence, (queries, new_keys, new_values, new_gates, kv_cache, gate_sums, live_lengths))
    attn_out = jnp.dot(attended, w_out, preferred_element_type=jnp.float32)
    after_mix = layer_norm(tokens.astype(jnp.float32) + attn_out, first_gain)
    gate_units = jnp.dot(after_mix, w_gate, preferred_element_type=jnp.float32)
    up_units = jnp.dot(after_mix, w_up, preferred_element_type=jnp.float32)
    hidden = (jax.nn.silu(gate_units) * up_units).astype(jnp.bfloat16)
    ffn_out = jnp.dot(hidden, w_down, preferred_element_type=jnp.float32)
    return layer_norm(after_mix.astype(jnp.float32) + ffn_out, second_gain)
```

```python
import jax
import jax.numpy as jnp
from jax import lax
from jax.experimental import pallas as pl
from jax.experimental.pallas import tpu as pltpu
from jax.sharding import PartitionSpec as P

MESH = pl.DeviceIdType.MESH
F32 = jnp.float32
BF16 = jnp.bfloat16

D = 4096
DH = 64
B = 16
X = 4
Z = 8
KV = 32
TP = 16
POS = 512
UNITS = 704
WIDE = 768
EPSILON = 1e-05
EMPTY_SCORE = -1e30
NT = (((1,), (1,)), ((), ()))


def iota(shape, dim):
    return lax.broadcasted_iota(jnp.int32, shape, dim)


def split3(v):
    hi = v.astype(BF16).astype(F32)
    rest = v - hi
    mid = rest.astype(BF16).astype(F32)
    return hi, mid, rest - mid


def nt(a, b):
    return lax.dot_general(a, b, NT, preferred_element_type=F32)


def lane_sum(v, lo, hi):
    lane = iota(v.shape, 1)
    return jnp.sum(jnp.where((lane >= lo) & (lane < hi), v, 0.0), axis=1, keepdims=True)


def kernel(
    lengths, bias, tok, g1, g2, kv_hbm, gs_hbm, wq_hbm, wk_hbm, wv_hbm, wf_hbm, wo_hbm, wg_hbm,
    wu_hbm, wd_hbm, out,
    cache, gs, wq, wkv, wf, wo, wg, wu, wd,
    tokv, gainv,
    b1, qx, qz, kx, kz, ax, az, b4, gm, bg, m5, b5, b6, b7, b8,
    qs, ngs, osum, otop, otot, pbuf, sbuf, gbuf,
    lsem, ssem, rsem,
):
    kv = lax.axis_index("kv")
    tp = lax.axis_index("tp")
    x = lax.rem(kv, X)
    z = kv // X

    loads = []

    def load(src, dst):
        c = pltpu.make_async_copy(src, dst, lsem.at[len(loads)])
        c.start()
        loads.append(c)
        return c

    l_tok = load(tok, tokv)
    l_g1 = load(g1, gainv.at[0])
    l_g2 = load(g2, gainv.at[1])
    l_wq = load(wq_hbm, wq)
    l_wk = load(wk_hbm, wkv.at[pl.ds(0, DH)])
    l_wv = load(wv_hbm, wkv.at[pl.ds(DH, DH)])
    l_wf = load(wf_hbm.at[:, pl.ds(pl.multiple_of(kv * 128, 128), 128)], wf)
    l_gs = load(gs_hbm, gs)
    l_kv = load(kv_hbm, cache)
    l_wg = load(wg_hbm, wg)
    l_wu = load(wu_hbm, wu)
    l_wo = load(wo_hbm, wo)
    l_wd = load(wd_hbm, wd.at[pl.ds(0, UNITS)])

    def kv_peer(i):
        a = lax.rem(kv + i, KV)
        return a, (a, tp)

    def x_peer(i):
        a = z * X + lax.rem(x + i, X)
        return a, (a, tp)

    def z_peer(i):
        a = lax.rem(kv + X * i, KV)
        return a, (a, tp)

    def tp_peer(i):
        a = lax.rem(tp + i, TP)
        return a, (kv, a)

    bar = pltpu.get_barrier_semaphore()

    def signal_kv(i, c):
        pl.semaphore_signal(bar, inc=1, device_id=kv_peer(i)[1], device_id_type=MESH)
        return c

    def signal_tp(i, c):
        pl.semaphore_signal(bar, inc=1, device_id=tp_peer(i)[1], device_id_type=MESH)
        return c

    lax.fori_loop(1, KV, signal_kv, 0)
    lax.fori_loop(1, TP, signal_tp, 0)

    waits = []
    used = [0]

    def exchange(n, peer, src_of, buf, slot):
        k = used[0]
        used[0] += 1

        def send(i, c):
            a, dev = peer(i)
            pltpu.make_async_remote_copy(
                src_ref=src_of(a), dst_ref=buf.at[slot], send_sem=ssem.at[k],
                recv_sem=rsem.at[k], device_id=dev, device_id_type=MESH,
            ).start()
            return c

        lax.fori_loop(1, n, send, 0, unroll=True)
        some = buf.at[pl.ds(0, n - 1)]
        waits.append(pltpu.make_async_copy(some, some, ssem.at[k]))
        return pltpu.make_async_copy(some, some, rsem.at[k])

    def spread(n, peer, buf, slot):
        return exchange(n, peer, lambda a: buf.at[slot], buf, slot)

    wd[pl.ds(UNITS, WIDE - UNITS), :] = jnp.zeros((WIDE - UNITS, 128), BF16)
    pbuf[...] = jnp.zeros_like(pbuf)
    gbuf[...] = jnp.zeros_like(gbuf)
    sbuf[...] = jnp.zeros_like(sbuf)
    gm[...] = jnp.zeros_like(gm)

    l_tok.wait()
    l_g1.wait()
    l_g2.wait()
    lane8 = iota((8, 128), 1)
    diag8 = iota((8, 8), 0) == iota((8, 8), 1)
    c1 = jnp.sum(jnp.where(diag8, gainv[0], 0.0), axis=1, keepdims=True)
    c2 = jnp.sum(jnp.where(diag8, gainv[1], 0.0), axis=1, keepdims=True)
    b1[tp] = jnp.where(lane8 == 16, c1, jnp.where(lane8 == 17, c2, 0.0))
    b1[tp, :, 0:B] = tokv[...].astype(F32)
    pl.semaphore_wait(bar, KV - 1 + TP - 1)
    r1 = spread(TP, tp_peer, b1, tp)
    l_wq.wait()
    l_wk.wait()
    l_wv.wait()
    l_wf.wait()
    r1.wait()
    turned = jnp.transpose(b1[...].reshape(128, 128))
    rows = turned[0:B, :]
    gain1 = turned[B : B + 1, :]
    gain2 = turned[B + 1 : B + 2, :]
    rows16 = rows.astype(BF16)

    lane = iota((B, 128), 1)
    q_part = jnp.dot(rows16, wq[...], preferred_element_type=F32)
    f_all = nt(rows16, wf[...])
    f_part = jnp.sum(jnp.where(iota((B, B), 1) == tp, f_all, 0.0), axis=1, keepdims=True)
    t_part = jnp.sum(rows, axis=1, keepdims=True)

    def small_tile(first, second):
        tile = jnp.zeros((B, 128), F32)
        for k, piece in enumerate((*split3(first), *split3(second))):
            tile = jnp.where(lane == k, piece, tile)
        return tile

    qx[x, 0:B] = q_part[:, 0:128].astype(BF16)
    qx[x, B : 2 * B] = q_part[:, 128:256].astype(BF16)
    qx[x, 2 * B : 3 * B] = small_tile(f_part, t_part).astype(BF16)
    r = spread(X, x_peer, qx, x)
    kx[x] = nt(rows16, wkv[...]).astype(BF16)
    rk = spread(X, x_peer, kx, x)
    r.wait()
    summed = jnp.sum(qx[...].astype(F32), axis=0)
    small = summed[2 * B : 3 * B]
    qz[z, 0 : 2 * B] = summed[0 : 2 * B].astype(BF16)
    qz[z, 2 * B : 3 * B] = small_tile(lane_sum(small, 0, 3), lane_sum(small, 3, 6)).astype(BF16)
    r = spread(Z, z_peer, qz, z)
    rk.wait()
    kz[z] = jnp.sum(kx[...].astype(F32), axis=0).astype(BF16)
    rk = spread(Z, z_peer, kz, z)

    l_wg.wait()
    l_wu.wait()
    row16 = iota((B, 128), 0)
    gh, gmid, gl = split3(gain1)
    gain_rows = jnp.where(
        row16 == 0, gh, jnp.where(row16 == 1, gmid, jnp.where(row16 == 2, gl, 0.0))
    ).astype(BF16)
    gbuf[0:1, 0:UNITS] = jnp.sum(nt(gain_rows, wg[...]), axis=0, keepdims=True)
    gbuf[1:2, 0:UNITS] = jnp.sum(nt(gain_rows, wu[...]), axis=0, keepdims=True)
    for h in range(2):
        for t in range(3):
            at = (h * 3 + t) * 128
            gm[h, t : t + 1, :] = gbuf[0:1, at : at + 128]
            gm[h, 3 + t : 4 + t, :] = gbuf[1:2, at : at + 128]
    half = lax.rem(kv, 2)
    bg[kv] = gm[half]
    l_gs.wait()
    l_kv.wait()

    r.wait()
    summed = jnp.sum(qz[...].astype(F32), axis=0)
    q0 = summed[0:B].astype(BF16).astype(F32)
    q1 = summed[B : 2 * B].astype(BF16).astype(F32)
    small = summed[2 * B : 3 * B]
    tok_mean = lane_sum(small, 3, 6) * (1.0 / D)
    gate_in = lane_sum(small, 0, 3) + bias[tp]
    new_gate = jnp.minimum(gate_in, 0.0) - jnp.log1p(jnp.exp(-jnp.abs(gate_in)))
    rg = exchange(KV, kv_peer, lambda a: gm.at[lax.rem(a, 2)], bg, kv)

    low = lane < DH
    qs[pl.ds(0, B, stride=4), :] = jnp.where(low, q0, 0.0)
    qs[pl.ds(1, B, stride=4), :] = jnp.where(low, pltpu.roll(q0, DH, 1), 0.0)
    qs[pl.ds(2, B, stride=4), :] = jnp.where(low, q1, 0.0)
    qs[pl.ds(3, B, stride=4), :] = jnp.where(low, pltpu.roll(q1, DH, 1), 0.0)
    gate_tile = jnp.broadcast_to(new_gate, (B, 128))
    for j in range(4):
        ngs[pl.ds(j, B, stride=4), :] = gate_tile
    scale = DH ** (-0.5)
    first = iota((8, POS), 0) < 4
    first128 = iota((8, 128), 0) < 4
    position = iota((8, POS), 1) + kv * POS
    for p in range(B // 2):
        own = pl.ds(8 * p, 8)
        queries = qs[own, :].astype(BF16)
        s = jnp.where(first, nt(queries, cache[2 * p]), nt(queries, cache[2 * p + 1])) * scale
        s = s + jnp.where(first, gs[2 * p], gs[2 * p + 1]) + ngs[own, 0:1]
        live = position < jnp.where(first, lengths[2 * p], lengths[2 * p + 1])
        top = jnp.max(jnp.where(live, s, EMPTY_SCORE), axis=1, keepdims=True)
        w = jnp.where(live, jnp.exp(s - top), 0.0)
        w16 = w.astype(BF16)
        osum[own, :] = jnp.where(
            first128,
            jnp.dot(w16, cache[2 * p], preferred_element_type=F32),
            jnp.dot(w16, cache[2 * p + 1], preferred_element_type=F32),
        )
        otop[own, :] = jnp.broadcast_to(top, (8, 128))
        otot[own, :] = jnp.broadcast_to(jnp.sum(w, axis=1, keepdims=True), (8, 128))

    def by_head(ref):
        return [ref[pl.ds(j, B, stride=4), :] for j in range(4)]

    os, tops, tots = by_head(osum), by_head(otop), by_head(otot)
    sums = [jnp.where(low, pltpu.roll(os[2 * i], DH, 1), os[2 * i + 1]) for i in range(2)]
    tops = [jnp.where(low, tops[2 * i], tops[2 * i + 1]) for i in range(2)]
    tots = [jnp.where(low, tots[2 * i], tots[2 * i + 1]) for i in range(2)]

    place = lax.rem(lane, DH)

    def pack(buf, slot):
        buf[slot, 0:B] = sums[0].astype(BF16)
        buf[slot, B : 2 * B] = sums[1].astype(BF16)
        tile = jnp.zeros((B, 128), F32)
        k = 0
        for v in (*tops, *tots):
            for piece in split3(v):
                tile = jnp.where(place == k, piece, tile)
                k += 1
        buf[slot, 2 * B : 3 * B] = tile.astype(BF16)

    src = iota((128, 512), 0)
    dst = iota((128, 512), 1)
    wanted = 3 * (dst // 128)
    pick = (src // DH == lax.rem(dst, 128) // DH) & (lax.rem(src, DH) >= wanted)
    pick = jnp.where(pick & (lax.rem(src, DH) < wanted + 3), 1.0, 0.0).astype(BF16)

    def unpack(buf, n):
        spreads = [
            jnp.dot(buf[i, 2 * B : 3 * B], pick, preferred_element_type=F32) for i in range(n)
        ]
        new_sums, new_tops, new_tots = [], [], []
        for c in range(2):
            t = [v[:, c * 128 : c * 128 + 128] for v in spreads]
            u = [v[:, 256 + c * 128 : 384 + c * 128] for v in spreads]
            top = t[0]
            for v in t[1:]:
                top = jnp.maximum(top, v)
            total, weighted = 0.0, 0.0
            for i in range(n):
                e = jnp.exp(t[i] - top)
                total = total + u[i] * e
                weighted = weighted + buf[i, c * B : c * B + B].astype(F32) * e
            new_sums.append(weighted)
            new_tops.append(top)
            new_tots.append(total)
        return new_sums, new_tops, new_tots

    pack(ax, x)
    r = spread(X, x_peer, ax, x)
    rk.wait()
    keyval = jnp.sum(kz[...].astype(F32), axis=0).astype(BF16).astype(F32)
    turned_kv = pltpu.roll(keyval, DH, 1)
    keys = jnp.where(low, keyval, turned_kv)
    values = jnp.where(low, turned_kv, keyval)
    owns = []
    for q in (q0, q1):
        prod = q * keys
        owns.append(jnp.where(low, lane_sum(prod, 0, DH), lane_sum(prod, DH, 128)) * scale)
    r.wait()
    sums, tops, tots = unpack(ax, X)
    pack(az, z)
    r = spread(Z, z_peer, az, z)
    rg.wait()
    gained = jnp.sum(bg[...], axis=0)
    l_wo.wait()
    r.wait()
    sums, tops, tots = unpack(az, Z)
    attended = []
    for c in range(2):
        final = jnp.maximum(tops[c], owns[c])
        carry = jnp.exp(tops[c] - final)
        own_weight = jnp.exp(owns[c] - final)
        top_part = sums[c] * carry + own_weight.astype(BF16).astype(F32) * values
        attended.append((top_part / (tots[c] * carry + own_weight)).astype(BF16))

    proj = jnp.dot(attended[0], wo[0:128, :], preferred_element_type=F32)
    proj = proj + jnp.dot(attended[1], wo[128:256, :], preferred_element_type=F32)
    b4[tp] = proj.astype(BF16)
    r = spread(TP, tp_peer, b4, tp)
    r.wait()
    centred = rows + jnp.sum(b4[...].astype(F32), axis=0) - tok_mean

    gained_rows = (centred * gain1).astype(BF16)
    stat = small_tile(
        jnp.sum(centred, axis=1, keepdims=True), jnp.sum(centred * centred, axis=1, keepdims=True)
    )
    for h in range(2):
        sbuf[pl.ds(h * 8 + 6, B, stride=16), :] = stat
    for which, w in enumerate((wg, wu)):
        pbuf[which, :, 0:UNITS] = nt(gained_rows, w[...])
        for h in range(2):
            for t in range(3):
                at = (h * 3 + t) * 128
                sbuf[pl.ds(h * 8 + which * 3 + t, B, stride=16), :] = pbuf[which, :, at : at + 128]
    m5[...] = sbuf[...].reshape(KV, 8, 128).astype(BF16)
    b5[kv] = m5[kv]
    r = exchange(KV, kv_peer, lambda a: m5.at[a], b5, kv)
    r.wait()
    units = jnp.sum(b5[...].astype(F32), axis=0)
    lane_row = iota((1, 128), 1)
    srow = units[6:7, :]
    mean = lane_sum(srow, 0, 3) * (1.0 / D)
    spread1 = lane_sum(srow, 3, 6) * (1.0 / D) - mean * mean
    rstd = lax.rsqrt(spread1 + EPSILON)
    units = (units - mean * gained) * rstd
    gates = units[0:3, :]
    hidden = gates / (1.0 + jnp.exp(-gates)) * units[3:6, :]
    b6[kv, 0:3, :] = hidden
    b6[kv, 3:4, :] = jnp.where(lane_row == 0, mean, jnp.where(lane_row == 1, rstd, 0.0))
    r = spread(KV, kv_peer, b6, kv)
    l_wd.wait()
    r.wait()
    flat = b6.reshape(KV * 4, 128)
    tiles = [
        flat[pl.ds(h * 4 + t, B, stride=8), :].astype(BF16) for h in range(2) for t in range(3)
    ]
    norms = flat[pl.ds(3, B, stride=8), :]
    down = jnp.dot(jnp.concatenate(tiles, axis=1), wd[...], preferred_element_type=F32)

    b7[tp] = down.astype(BF16)
    r = spread(TP, tp_peer, b7, tp)
    mid = (centred - lane_sum(norms, 0, 1)) * lane_sum(norms, 1, 2) * gain1
    mid = mid.astype(BF16).astype(F32)
    r.wait()
    mixed = mid + jnp.sum(b7[...].astype(F32), axis=0)

    sum2 = jnp.sum(mixed, axis=1, keepdims=True)
    off = mixed - sum2 * (1.0 / 128)
    square2 = jnp.sum(off * off, axis=1, keepdims=True)
    stat = jnp.where(lane == row16, sum2, jnp.where(lane == row16 + B, square2, 0.0))
    b8[kv] = jnp.sum(stat, axis=0, keepdims=True)
    r = spread(KV, kv_peer, b8, kv)
    r.wait()
    stats = b8[...].reshape(KV, 128)
    total2 = jnp.sum(stats, axis=0, keepdims=True)
    drift = stats * (1.0 / 128) - total2 * (1.0 / D)
    between = jnp.sum(drift * drift, axis=0, keepdims=True) * 128.0
    mean2 = jnp.sum(jnp.where(lane == row16, total2, 0.0), axis=1, keepdims=True) * (1.0 / D)
    var2 = jnp.sum(
        jnp.where(lane == row16, between, jnp.where(lane == row16 + B, total2, 0.0)),
        axis=1, keepdims=True,
    ) * (1.0 / D)
    result = ((mixed - mean2) * lax.rsqrt(var2 + EPSILON) * gain2).astype(BF16)
    chosen = jnp.where(iota((8, 128), 1) == iota((8, 128), 0) + tp * 8, 1.0, 0.0).astype(BF16)
    out[...] = nt(chosen, result).astype(BF16)
    for w in waits:
        w.wait()


def on_device(
    tokens, live_lengths, kv_cache, gate_sums, w_query, w_key, w_value, w_forget, forget_bias,
    w_out, first_gain, w_gate, w_up, w_down, second_gain,
):
    smem = pl.BlockSpec(memory_space=pltpu.SMEM)
    hbm = pl.BlockSpec(memory_space=pl.ANY)
    vmem = pltpu.VMEM
    turned = pl.pallas_call(
        kernel,
        out_shape=jax.ShapeDtypeStruct((8, B), BF16),
        in_specs=[smem, smem] + [hbm] * 13,
        out_specs=pl.BlockSpec(memory_space=pltpu.VMEM),
        scratch_shapes=[
            vmem((B, POS, 128), BF16),
            vmem((B, 1, POS), F32),
            vmem((128, 256), BF16),
            vmem((128, 128), BF16),
            vmem((16, 128), BF16),
            vmem((256, 128), BF16),
            vmem((UNITS, 128), BF16),
            vmem((UNITS, 128), BF16),
            vmem((WIDE, 128), BF16),
            vmem((8, B), BF16),
            vmem((2, 1, 8), F32),
            vmem((TP, 8, 128), F32),
            vmem((X, 3 * B, 128), BF16),
            vmem((Z, 3 * B, 128), BF16),
            vmem((X, B, 128), BF16),
            vmem((Z, B, 128), BF16),
            vmem((X, 3 * B, 128), BF16),
            vmem((Z, 3 * B, 128), BF16),
            vmem((TP, B, 128), BF16),
            vmem((2, 8, 128), F32),
            vmem((KV, 8, 128), F32),
            vmem((KV, 8, 128), BF16),
            vmem((KV, 8, 128), BF16),
            vmem((KV, 4, 128), F32),
            vmem((TP, B, 128), BF16),
            vmem((KV, 1, 128), F32),
            vmem((64, 128), F32),
            vmem((64, 128), F32),
            vmem((64, 128), F32),
            vmem((64, 128), F32),
            vmem((64, 128), F32),
            vmem((2, B, WIDE), F32),
            vmem((KV * 8, 128), F32),
            vmem((2, WIDE), F32),
            pltpu.SemaphoreType.DMA((13,)),
            pltpu.SemaphoreType.DMA((13,)),
            pltpu.SemaphoreType.DMA((13,)),
        ],
        compiler_params=pltpu.CompilerParams(collective_id=0, has_side_effects=True),
    )(
        live_lengths, forget_bias, tokens.T, first_gain.reshape(1, 8), second_gain.reshape(1, 8),
        kv_cache, gate_sums, w_query, w_key.T, w_value.T, w_forget.T, w_out, w_gate.T, w_up.T,
        w_down,
    )
    return turned.T


def solution(mesh):
    placed = (
        P(None, ("kv", "tp")), P(), P(None, "kv", "tp"), P(None, "tp", "kv"), P("kv", "tp"),
        P("kv", "tp"), P("kv", "tp"), P(), P(), P("tp", "kv"), P(("kv", "tp")), P("kv", "tp"),
        P("kv", "tp"), P("tp", "kv"), P(("kv", "tp")),
    )
    return jax.shard_map(
        on_device, mesh=mesh, in_specs=placed, out_specs=P(None, ("kv", "tp")), check_vma=False
    )
```

```python
import jax
import jax.numpy as jnp
from jax import lax
from jax.experimental import pallas as pl
from jax.experimental.pallas import tpu as pltpu
from jax.sharding import PartitionSpec as P

MESH = pl.DeviceIdType.MESH
F32 = jnp.float32
BF16 = jnp.bfloat16

D = 4096
DH = 64
B = 16
X = 4
Z = 8
KV = 32
TP = 16
POS = 512
UNITS = 704
WIDE = 768
EPSILON = 1e-05
EMPTY_SCORE = -1e30


def hops(o, sizes):
    return sum(min(d, n - d) for d, n in zip(o, sizes))


def far_first(sizes):
    offsets = [(i, j) for i in range(sizes[0]) for j in range(sizes[1]) if i or j]
    return sorted(offsets, key=lambda o: -hops(o, sizes))


X_FAR = [2, 1, 3]
Z_FAR = [4, 3, 5, 2, 6, 1, 7]
KV_FAR = far_first((Z, X))
TP_FAR = far_first((TP // 2, 2))
NT = (((1,), (1,)), ((), ()))


def iota(shape, dim):
    return lax.broadcasted_iota(jnp.int32, shape, dim)


def split3(v):
    hi = v.astype(BF16).astype(F32)
    rest = v - hi
    mid = rest.astype(BF16).astype(F32)
    return hi, mid, rest - mid


def nt(a, b):
    return lax.dot_general(a, b, NT, preferred_element_type=F32)


def lane_sum(v, lo, hi):
    lane = iota(v.shape, 1)
    return jnp.sum(jnp.where((lane >= lo) & (lane < hi), v, 0.0), axis=1, keepdims=True)


def kernel(
    lengths_hbm, bias_hbm, tok, g1, g2, kv_hbm, gs_hbm, wq_hbm, wk_hbm, wv_hbm, wf_hbm, wo_hbm, wg_hbm,
    wu_hbm, wd_hbm, out,
    cache, gs, wq, wkv, wf, wo, wg, wu, wd,
    tokv, gainv,
    b1, qx, qz, kx, kz, ax, az, b4, gm, bg, m5, b5, b6, b7, b8,
    qs, ngs, scores, weights, osum, otop, otot, pbuf, sbuf, gbuf,
    lengths, bias, lsem, ssem, rsem,
):
    kv = lax.axis_index("kv")
    tp = lax.axis_index("tp")
    x = lax.rem(kv, X)
    z = kv // X

    def kv_peer(o):
        a = lax.rem(z + o[0], Z) * X + lax.rem(x + o[1], X)
        return a, (a, tp)

    def x_peer(o):
        a = z * X + lax.rem(x + o, X)
        return a, (a, tp)

    def z_peer(o):
        a = lax.rem(kv + X * o, KV)
        return a, (a, tp)

    def tp_peer(o):
        a = lax.rem(tp // 2 + o[0], TP // 2) * 2 + lax.rem(tp + o[1], 2)
        return a, (kv, a)

    bar = pltpu.get_barrier_semaphore()
    greeted = [(tp_peer, o) for o in TP_FAR] + [(z_peer, o) for o in Z_FAR]
    greeted += [(x_peer, o) for o in X_FAR]
    for peer, o in greeted:
        pl.semaphore_signal(bar, inc=1, device_id=peer(o)[1], device_id_type=MESH)

    loads = []

    def load(src, dst):
        c = pltpu.make_async_copy(src, dst, lsem.at[len(loads)])
        c.start()
        loads.append(c)
        return c

    l_tok = load(tok, tokv)
    l_g1 = load(g1, gainv.at[0])
    l_g2 = load(g2, gainv.at[1])
    l_len = load(lengths_hbm, lengths)
    l_bias = load(bias_hbm, bias)
    l_wq = load(wq_hbm, wq)
    l_wk = load(wk_hbm, wkv.at[pl.ds(0, DH)])
    l_wv = load(wv_hbm, wkv.at[pl.ds(DH, DH)])
    l_wf = load(wf_hbm.at[:, pl.ds(pl.multiple_of(kv * 128, 128), 128)], wf)
    l_gs = load(gs_hbm, gs)
    l_kv = load(kv_hbm, cache)
    l_wg = load(wg_hbm, wg)
    l_wu = load(wu_hbm, wu)
    l_wo = load(wo_hbm, wo)
    l_wd = load(wd_hbm, wd.at[pl.ds(0, UNITS)])

    waits = []
    used = [0]

    def exchange(far, peer, src_of, buf, slot):
        k = used[0]
        used[0] += 1
        for o in far:
            a, dev = peer(o)
            pltpu.make_async_remote_copy(
                src_ref=src_of(a), dst_ref=buf.at[slot], send_sem=ssem.at[k],
                recv_sem=rsem.at[k], device_id=dev, device_id_type=MESH,
            ).start()
        some = buf.at[pl.ds(0, len(far))]
        waits.append(pltpu.make_async_copy(some, some, ssem.at[k]))
        return pltpu.make_async_copy(some, some, rsem.at[k])

    def spread(far, peer, buf, slot):
        return exchange(far, peer, lambda a: buf.at[slot], buf, slot)

    wd[pl.ds(UNITS, WIDE - UNITS), :] = jnp.zeros((WIDE - UNITS, 128), BF16)
    pbuf[...] = jnp.zeros_like(pbuf)
    gbuf[...] = jnp.zeros_like(gbuf)
    sbuf[...] = jnp.zeros_like(sbuf)
    gm[...] = jnp.zeros_like(gm)

    l_tok.wait()
    l_g1.wait()
    l_g2.wait()
    lane8 = iota((8, 128), 1)
    diag8 = iota((8, 8), 0) == iota((8, 8), 1)
    c1 = jnp.sum(jnp.where(diag8, gainv[0], 0.0), axis=1, keepdims=True)
    c2 = jnp.sum(jnp.where(diag8, gainv[1], 0.0), axis=1, keepdims=True)
    b1[tp] = jnp.where(lane8 == 16, c1, jnp.where(lane8 == 17, c2, 0.0))
    b1[tp, :, 0:B] = tokv[...].astype(F32)
    pl.semaphore_wait(bar, len(greeted))
    r1 = spread(TP_FAR, tp_peer, b1, tp)
    l_wq.wait()
    l_wk.wait()
    l_wv.wait()
    l_wf.wait()
    r1.wait()
    turned = jnp.transpose(b1[...].reshape(128, 128))
    rows = turned[0:B, :]
    gain1 = turned[B : B + 1, :]
    gain2 = turned[B + 1 : B + 2, :]
    rows16 = rows.astype(BF16)

    scale = DH ** (-0.5)
    lane = iota((B, 128), 1)
    q_part = jnp.dot(rows16, wq[...], preferred_element_type=F32)
    f_all = nt(rows16, wf[...])
    f_part = jnp.sum(jnp.where(iota((B, B), 1) == tp, f_all, 0.0), axis=1, keepdims=True)
    t_part = jnp.sum(rows, axis=1, keepdims=True)

    def small_tile(first, second):
        tile = jnp.zeros((B, 128), F32)
        for k, piece in enumerate((*split3(first), *split3(second))):
            tile = jnp.where(lane == k, piece, tile)
        return tile

    qx[x, 0:B] = q_part[:, 0:128].astype(BF16)
    qx[x, B : 2 * B] = q_part[:, 128:256].astype(BF16)
    qx[x, 2 * B : 3 * B] = small_tile(f_part, t_part).astype(BF16)
    r = spread(X_FAR, x_peer, qx, x)
    kx[x] = nt(rows16, wkv[...]).astype(BF16)
    rk = spread(X_FAR, x_peer, kx, x)
    r.wait()
    summed = jnp.sum(qx[...].astype(F32), axis=0)
    small = summed[2 * B : 3 * B]
    qz[z, 0 : 2 * B] = summed[0 : 2 * B].astype(BF16)
    qz[z, 2 * B : 3 * B] = small_tile(lane_sum(small, 0, 3), lane_sum(small, 3, 6)).astype(BF16)
    r = spread(Z_FAR, z_peer, qz, z)
    rk.wait()
    kz[z] = jnp.sum(kx[...].astype(F32), axis=0).astype(BF16)
    rk = spread(Z_FAR, z_peer, kz, z)

    l_wg.wait()
    l_wu.wait()
    row16 = iota((B, 128), 0)
    gh, gmid, gl = split3(gain1)
    gain_rows = jnp.where(
        row16 == 0, gh, jnp.where(row16 == 1, gmid, jnp.where(row16 == 2, gl, 0.0))
    ).astype(BF16)
    gbuf[0:1, 0:UNITS] = jnp.sum(nt(gain_rows, wg[...]), axis=0, keepdims=True)
    gbuf[1:2, 0:UNITS] = jnp.sum(nt(gain_rows, wu[...]), axis=0, keepdims=True)
    for h in range(2):
        for t in range(3):
            at = (h * 3 + t) * 128
            gm[h, t : t + 1, :] = gbuf[0:1, at : at + 128]
            gm[h, 3 + t : 4 + t, :] = gbuf[1:2, at : at + 128]
    half = lax.rem(kv, 2)
    bg[kv] = gm[half]
    l_gs.wait()
    l_kv.wait()
    l_len.wait()
    l_bias.wait()

    r.wait()
    summed = jnp.sum(qz[...].astype(F32), axis=0)
    q0 = summed[0:B].astype(BF16).astype(F32)
    q1 = summed[B : 2 * B].astype(BF16).astype(F32)
    q0, q1 = q0 * scale, q1 * scale
    small = summed[2 * B : 3 * B]
    tok_mean = lane_sum(small, 3, 6) * (1.0 / D)
    gate_in = lane_sum(small, 0, 3) + bias[tp]
    new_gate = jnp.minimum(gate_in, 0.0) - jnp.log1p(jnp.exp(-jnp.abs(gate_in)))
    rg = exchange(KV_FAR, kv_peer, lambda a: gm.at[lax.rem(a, 2)], bg, kv)

    low = lane < DH
    qs[pl.ds(0, B, stride=4), :] = jnp.where(low, q0, 0.0)
    qs[pl.ds(1, B, stride=4), :] = jnp.where(low, pltpu.roll(q0, DH, 1), 0.0)
    qs[pl.ds(2, B, stride=4), :] = jnp.where(low, q1, 0.0)
    qs[pl.ds(3, B, stride=4), :] = jnp.where(low, pltpu.roll(q1, DH, 1), 0.0)
    gate_tile = jnp.broadcast_to(new_gate, (B, 128))
    for j in range(4):
        ngs[pl.ds(j, B, stride=4), :] = gate_tile
    first = iota((8, POS), 0) < 4
    first128 = iota((8, 128), 0) < 4
    position = iota((8, POS), 1) + kv * POS
    for p in range(B // 2):
        own = pl.ds(8 * p, 8)
        queries = qs[own, :].astype(BF16)
        s = jnp.where(first, nt(queries, cache[2 * p]), nt(queries, cache[2 * p + 1]))
        s = s + jnp.where(first, gs[2 * p], gs[2 * p + 1]) + ngs[own, 0:1]
        live = position < jnp.where(first, lengths[2 * p], lengths[2 * p + 1])
        scores[own, :] = jnp.where(live, s, EMPTY_SCORE)
    s = scores[...]
    top = jnp.max(s, axis=1, keepdims=True)
    w = jnp.where(s > 0.5 * EMPTY_SCORE, jnp.exp(s - top), 0.0)
    otop[...] = jnp.broadcast_to(top, (64, 128))
    otot[...] = jnp.broadcast_to(jnp.sum(w, axis=1, keepdims=True), (64, 128))
    weights[...] = w.astype(BF16)
    for p in range(B // 2):
        own = pl.ds(8 * p, 8)
        w16 = weights[own, :]
        osum[own, :] = jnp.where(
            first128,
            jnp.dot(w16, cache[2 * p], preferred_element_type=F32),
            jnp.dot(w16, cache[2 * p + 1], preferred_element_type=F32),
        )

    def by_head(ref):
        return [ref[pl.ds(j, B, stride=4), :] for j in range(4)]

    os, tops, tots = by_head(osum), by_head(otop), by_head(otot)
    sums = [jnp.where(low, pltpu.roll(os[2 * i], DH, 1), os[2 * i + 1]) for i in range(2)]
    tops = [jnp.where(low, tops[2 * i], tops[2 * i + 1]) for i in range(2)]
    tots = [jnp.where(low, tots[2 * i], tots[2 * i + 1]) for i in range(2)]

    place = lax.rem(lane, DH)

    def pack(buf, slot):
        buf[slot, 0:B] = sums[0].astype(BF16)
        buf[slot, B : 2 * B] = sums[1].astype(BF16)
        tile = jnp.zeros((B, 128), F32)
        k = 0
        for v in (*tops, *tots):
            for piece in split3(v):
                tile = jnp.where(place == k, piece, tile)
                k += 1
        buf[slot, 2 * B : 3 * B] = tile.astype(BF16)

    src = iota((128, 512), 0)
    dst = iota((128, 512), 1)
    wanted = 3 * (dst // 128)
    pick = (src // DH == lax.rem(dst, 128) // DH) & (lax.rem(src, DH) >= wanted)
    pick = jnp.where(pick & (lax.rem(src, DH) < wanted + 3), 1.0, 0.0).astype(BF16)

    def unpack(buf, n):
        spreads = [
            jnp.dot(buf[i, 2 * B : 3 * B], pick, preferred_element_type=F32) for i in range(n)
        ]
        new_sums, new_tops, new_tots = [], [], []
        for c in range(2):
            t = [v[:, c * 128 : c * 128 + 128] for v in spreads]
            u = [v[:, 256 + c * 128 : 384 + c * 128] for v in spreads]
            top = t[0]
            for v in t[1:]:
                top = jnp.maximum(top, v)
            total, weighted = 0.0, 0.0
            for i in range(n):
                e = jnp.exp(t[i] - top)
                total = total + u[i] * e
                weighted = weighted + buf[i, c * B : c * B + B].astype(F32) * e
            new_sums.append(weighted)
            new_tops.append(top)
            new_tots.append(total)
        return new_sums, new_tops, new_tots

    pack(ax, x)
    r = spread(X_FAR, x_peer, ax, x)
    rk.wait()
    keyval = jnp.sum(kz[...].astype(F32), axis=0).astype(BF16).astype(F32)
    turned_kv = pltpu.roll(keyval, DH, 1)
    keys = jnp.where(low, keyval, turned_kv)
    values = jnp.where(low, turned_kv, keyval)
    owns = []
    for q in (q0, q1):
        prod = q * keys
        owns.append(jnp.where(low, lane_sum(prod, 0, DH), lane_sum(prod, DH, 128)))
    r.wait()
    sums, tops, tots = unpack(ax, X)
    pack(az, z)
    r = spread(Z_FAR, z_peer, az, z)
    rg.wait()
    gained = jnp.sum(bg[...], axis=0)
    l_wo.wait()
    r.wait()
    sums, tops, tots = unpack(az, Z)
    attended = []
    for c in range(2):
        final = jnp.maximum(tops[c], owns[c])
        carry = jnp.exp(tops[c] - final)
        own_weight = jnp.exp(owns[c] - final)
        top_part = sums[c] * carry + own_weight.astype(BF16).astype(F32) * values
        attended.append((top_part / (tots[c] * carry + own_weight)).astype(BF16))

    proj = jnp.dot(attended[0], wo[0:128, :], preferred_element_type=F32)
    proj = proj + jnp.dot(attended[1], wo[128:256, :], preferred_element_type=F32)
    b4[tp] = proj.astype(BF16)
    r = spread(TP_FAR, tp_peer, b4, tp)
    r.wait()
    centred = rows + jnp.sum(b4[...].astype(F32), axis=0) - tok_mean

    gained_rows = (centred * gain1).astype(BF16)
    stat = small_tile(
        jnp.sum(centred, axis=1, keepdims=True), jnp.sum(centred * centred, axis=1, keepdims=True)
    )
    for h in range(2):
        sbuf[pl.ds(h * 8 + 6, B, stride=16), :] = stat
    for which, w in enumerate((wg, wu)):
        pbuf[which, :, 0:UNITS] = nt(gained_rows, w[...])
        for h in range(2):
            for t in range(3):
                at = (h * 3 + t) * 128
                sbuf[pl.ds(h * 8 + which * 3 + t, B, stride=16), :] = pbuf[which, :, at : at + 128]
    m5[...] = sbuf[...].reshape(KV, 8, 128).astype(BF16)
    b5[kv] = m5[kv]
    r = exchange(KV_FAR, kv_peer, lambda a: m5.at[a], b5, kv)
    r.wait()
    units = jnp.sum(b5[...].astype(F32), axis=0)
    lane_row = iota((1, 128), 1)
    srow = units[6:7, :]
    mean = lane_sum(srow, 0, 3) * (1.0 / D)
    spread1 = lane_sum(srow, 3, 6) * (1.0 / D) - mean * mean
    rstd = lax.rsqrt(spread1 + EPSILON)
    units = (units - mean * gained) * rstd
    gates = units[0:3, :]
    hidden = gates / (1.0 + jnp.exp(-gates)) * units[3:6, :]
    b6[kv, 0:3, :] = hidden
    b6[kv, 3:4, :] = jnp.where(lane_row == 0, mean, jnp.where(lane_row == 1, rstd, 0.0))
    r = spread(KV_FAR, kv_peer, b6, kv)
    l_wd.wait()
    r.wait()
    flat = b6.reshape(KV * 4, 128)
    tiles = [
        flat[pl.ds(h * 4 + t, B, stride=8), :].astype(BF16) for h in range(2) for t in range(3)
    ]
    norms = flat[pl.ds(3, B, stride=8), :]
    down = jnp.dot(jnp.concatenate(tiles, axis=1), wd[...], preferred_element_type=F32)

    b7[tp] = down.astype(BF16)
    r = spread(TP_FAR, tp_peer, b7, tp)
    mid = (centred - lane_sum(norms, 0, 1)) * lane_sum(norms, 1, 2) * gain1
    mid = mid.astype(BF16).astype(F32)
    r.wait()
    mixed = mid + jnp.sum(b7[...].astype(F32), axis=0)

    sum2 = jnp.sum(mixed, axis=1, keepdims=True)
    off = mixed - sum2 * (1.0 / 128)
    square2 = jnp.sum(off * off, axis=1, keepdims=True)
    stat = jnp.where(lane == row16, sum2, jnp.where(lane == row16 + B, square2, 0.0))
    b8[kv] = jnp.sum(stat, axis=0, keepdims=True)
    r = spread(KV_FAR, kv_peer, b8, kv)
    r.wait()
    stats = b8[...].reshape(KV, 128)
    total2 = jnp.sum(stats, axis=0, keepdims=True)
    drift = stats * (1.0 / 128) - total2 * (1.0 / D)
    between = jnp.sum(drift * drift, axis=0, keepdims=True) * 128.0
    mean2 = jnp.sum(jnp.where(lane == row16, total2, 0.0), axis=1, keepdims=True) * (1.0 / D)
    var2 = jnp.sum(
        jnp.where(lane == row16, between, jnp.where(lane == row16 + B, total2, 0.0)),
        axis=1, keepdims=True,
    ) * (1.0 / D)
    result = ((mixed - mean2) * lax.rsqrt(var2 + EPSILON) * gain2).astype(BF16)
    chosen = jnp.where(iota((8, 128), 1) == iota((8, 128), 0) + tp * 8, 1.0, 0.0).astype(BF16)
    out[...] = nt(chosen, result).astype(BF16)
    for w in waits:
        w.wait()


def on_device(
    tokens, live_lengths, kv_cache, gate_sums, w_query, w_key, w_value, w_forget, forget_bias,
    w_out, first_gain, w_gate, w_up, w_down, second_gain,
):
    hbm = pl.BlockSpec(memory_space=pl.ANY)
    vmem = pltpu.VMEM
    turned = pl.pallas_call(
        kernel,
        out_shape=jax.ShapeDtypeStruct((8, B), BF16),
        in_specs=[hbm] * 15,
        out_specs=pl.BlockSpec(memory_space=pltpu.VMEM),
        scratch_shapes=[
            vmem((B, POS, 128), BF16),
            vmem((B, 1, POS), F32),
            vmem((128, 256), BF16),
            vmem((128, 128), BF16),
            vmem((16, 128), BF16),
            vmem((256, 128), BF16),
            vmem((UNITS, 128), BF16),
            vmem((UNITS, 128), BF16),
            vmem((WIDE, 128), BF16),
            vmem((8, B), BF16),
            vmem((2, 1, 8), F32),
            vmem((TP, 8, 128), F32),
            vmem((X, 3 * B, 128), BF16),
            vmem((Z, 3 * B, 128), BF16),
            vmem((X, B, 128), BF16),
            vmem((Z, B, 128), BF16),
            vmem((X, 3 * B, 128), BF16),
            vmem((Z, 3 * B, 128), BF16),
            vmem((TP, B, 128), BF16),
            vmem((2, 8, 128), F32),
            vmem((KV, 8, 128), F32),
            vmem((KV, 8, 128), BF16),
            vmem((KV, 8, 128), BF16),
            vmem((KV, 4, 128), F32),
            vmem((TP, B, 128), BF16),
            vmem((KV, 1, 128), F32),
            vmem((64, 128), F32),
            vmem((64, 128), F32),
            vmem((64, POS), F32),
            vmem((64, POS), BF16),
            vmem((64, 128), F32),
            vmem((64, 128), F32),
            vmem((64, 128), F32),
            vmem((2, B, WIDE), F32),
            vmem((KV * 8, 128), F32),
            vmem((2, WIDE), F32),
            pltpu.SMEM((B,), jnp.int32),
            pltpu.SMEM((TP,), F32),
            pltpu.SemaphoreType.DMA((15,)),
            pltpu.SemaphoreType.DMA((13,)),
            pltpu.SemaphoreType.DMA((13,)),
        ],
        compiler_params=pltpu.CompilerParams(collective_id=0, has_side_effects=True),
    )(
        live_lengths, forget_bias, tokens.T, first_gain.reshape(1, 8), second_gain.reshape(1, 8),
        kv_cache, gate_sums, w_query, w_key.T, w_value.T, w_forget.T, w_out, w_gate.T, w_up.T,
        w_down,
    )
    return turned.T


def solution(mesh):
    placed = (
        P(None, ("kv", "tp")), P(), P(None, "kv", "tp"), P(None, "tp", "kv"), P("kv", "tp"),
        P("kv", "tp"), P("kv", "tp"), P(), P(), P("tp", "kv"), P(("kv", "tp")), P("kv", "tp"),
        P("kv", "tp"), P("tp", "kv"), P(("kv", "tp")),
    )
    return jax.shard_map(
        on_device, mesh=mesh, in_specs=placed, out_specs=P(None, ("kv", "tp")), check_vma=False
    )
```

```python
import jax
import jax.numpy as jnp
from jax import lax
from jax.experimental import pallas as pl
from jax.experimental.pallas import tpu as pltpu
from jax.sharding import PartitionSpec as P

MESH = pl.DeviceIdType.MESH
F32 = jnp.float32
BF16 = jnp.bfloat16

D = 4096
DH = 64
B = 16
X = 4
Z = 8
KV = 32
TP = 16
POS = 512
UNITS = 704
WIDE = 768
EPSILON = 1e-05
EMPTY_SCORE = -1e30


def hops(o, sizes):
    return sum(min(d, n - d) for d, n in zip(o, sizes))


def far_first(sizes):
    offsets = [(i, j) for i in range(sizes[0]) for j in range(sizes[1]) if i or j]
    return sorted(offsets, key=lambda o: -hops(o, sizes))


X_FAR = [2, 1, 3]
Z_FAR = [4, 3, 5, 2, 6, 1, 7]
KV_FAR = far_first((Z, X))
TP_FAR = far_first((TP // 2, 2))
NT = (((1,), (1,)), ((), ()))


def iota(shape, dim):
    return lax.broadcasted_iota(jnp.int32, shape, dim)


def split3(v):
    hi = v.astype(BF16).astype(F32)
    rest = v - hi
    mid = rest.astype(BF16).astype(F32)
    return hi, mid, rest - mid


def nt(a, b):
    return lax.dot_general(a, b, NT, preferred_element_type=F32)


def lane_sum(v, lo, hi):
    lane = iota(v.shape, 1)
    return jnp.sum(jnp.where((lane >= lo) & (lane < hi), v, 0.0), axis=1, keepdims=True)


def kernel(
    lengths_hbm, bias_hbm, tok, g1, g2, kv_hbm, gs_hbm, wq_hbm, wk_hbm, wv_hbm, wf_hbm, wo_hbm, wg_hbm,
    wu_hbm, wd_hbm, out,
    cache, gs, wq, wkv, wf, wo, wg, wu, wd,
    tokv, gainv,
    b1, qa, qb, pairs, m2, b2, aa, ab, sa, sb, b4, gm, bg, m5, b5, b6, b7, b8,
    qs, ngs, scores, weights, osum, otop, otot, pbuf, sbuf, gbuf, gtile,
    lengths, bias, plane, lsem, ssem, rsem,
):
    kv = lax.axis_index("kv")
    tp = lax.axis_index("tp")
    x = lax.rem(kv, X)
    z = kv // X

    def kv_peer(o):
        a = lax.rem(z + o[0], Z) * X + lax.rem(x + o[1], X)
        return a, (a, tp)

    def x_peer(o):
        a = z * X + lax.rem(x + o, X)
        return a, (a, tp)

    def z_peer(o):
        a = lax.rem(kv + X * o, KV)
        return a, (a, tp)

    def tp_peer(o):
        a = lax.rem(tp // 2 + o[0], TP // 2) * 2 + lax.rem(tp + o[1], 2)
        return a, (kv, a)

    bar = pltpu.get_barrier_semaphore()
    greeted = [(tp_peer, o) for o in TP_FAR] + [(z_peer, o) for o in Z_FAR]
    greeted += [(x_peer, o) for o in X_FAR]
    for peer, o in greeted:
        pl.semaphore_signal(bar, inc=1, device_id=peer(o)[1], device_id_type=MESH)

    loads = []

    def load(src, dst):
        c = pltpu.make_async_copy(src, dst, lsem.at[len(loads)])
        c.start()
        loads.append(c)
        return c

    l_tok = load(tok, tokv)
    l_g1 = load(g1, gainv.at[0])
    l_g2 = load(g2, gainv.at[1])
    l_len = load(lengths_hbm, lengths)
    l_bias = load(bias_hbm, bias)
    l_wq = load(wq_hbm, wq)
    l_wk = load(wk_hbm, wkv.at[pl.ds(0, DH)])
    l_wv = load(wv_hbm, wkv.at[pl.ds(DH, DH)])
    l_wf = load(wf_hbm.at[:, pl.ds(pl.multiple_of(kv * 128, 128), 128)], wf)
    l_gs = load(gs_hbm, gs)
    l_kv = load(kv_hbm, cache)
    l_wg = load(wg_hbm, wg)
    l_wu = load(wu_hbm, wu)
    l_wo = load(wo_hbm, wo)
    l_wd = load(wd_hbm, wd.at[pl.ds(0, UNITS)])

    waits = []
    used = [0]

    def both(far, peer, pieces, slot):
        k = used[0]
        used[0] += len(pieces)
        for o in far:
            a, dev = peer(o)
            for n, (src_of, buf) in enumerate(pieces):
                pltpu.make_async_remote_copy(
                    src_ref=src_of(a), dst_ref=buf.at[slot], send_sem=ssem.at[k + n],
                    recv_sem=rsem.at[k + n], device_id=dev, device_id_type=MESH,
                ).start()
        got = []
        for n, (_, buf) in enumerate(pieces):
            some = buf.at[pl.ds(0, len(far))]
            waits.append(pltpu.make_async_copy(some, some, ssem.at[k + n]))
            got.append(pltpu.make_async_copy(some, some, rsem.at[k + n]))
        return got

    def exchange(far, peer, src_of, buf, slot):
        return both(far, peer, ((src_of, buf),), slot)[0]

    def spread(far, peer, buf, slot):
        return exchange(far, peer, lambda a: buf.at[slot], buf, slot)

    wd[pl.ds(UNITS, WIDE - UNITS), :] = jnp.zeros((WIDE - UNITS, 128), BF16)
    pbuf[...] = jnp.zeros_like(pbuf)
    gbuf[...] = jnp.zeros_like(gbuf)
    sbuf[...] = jnp.zeros_like(sbuf)
    gtile[...] = jnp.zeros_like(gtile)

    l_tok.wait()
    l_g1.wait()
    l_g2.wait()
    lane8 = iota((8, 128), 1)
    diag8 = iota((8, 8), 0) == iota((8, 8), 1)
    c1 = jnp.sum(jnp.where(diag8, gainv[0], 0.0), axis=1, keepdims=True)
    c2 = jnp.sum(jnp.where(diag8, gainv[1], 0.0), axis=1, keepdims=True)
    b1[tp] = jnp.where(lane8 == 16, c1, jnp.where(lane8 == 17, c2, 0.0))
    b1[tp, :, 0:B] = tokv[...].astype(F32)
    pl.semaphore_wait(bar, len(greeted))
    for o in X_FAR:
        pl.semaphore_signal(plane, inc=1, device_id=x_peer(o)[1], device_id_type=MESH)
    r1 = spread(TP_FAR, tp_peer, b1, tp)
    l_wq.wait()
    l_wk.wait()
    l_wv.wait()
    l_wf.wait()
    r1.wait()
    turned = jnp.transpose(b1[...].reshape(128, 128))
    rows = turned[0:B, :]
    gain1 = turned[B : B + 1, :]
    gain2 = turned[B + 1 : B + 2, :]
    rows16 = rows.astype(BF16)

    scale = DH ** (-0.5)
    lane = iota((B, 128), 1)
    q_part = jnp.dot(rows16, wq[...], preferred_element_type=F32)
    f_all = nt(rows16, wf[...])
    f_part = jnp.sum(jnp.where(iota((B, B), 1) == tp, f_all, 0.0), axis=1, keepdims=True)
    t_part = jnp.sum(rows, axis=1, keepdims=True)

    def small_tile(first, second):
        tile = jnp.zeros((B, 128), F32)
        for k, piece in enumerate((*split3(first), *split3(second))):
            tile = jnp.where(lane == k, piece, tile)
        return tile

    for half, buf in enumerate((qa, qb)):
        few = slice(8 * half, 8 * half + 8)
        buf[kv] = jnp.concatenate([q_part[few, 0:128], q_part[few, 128:256]], axis=0).astype(BF16)
    pl.semaphore_wait(plane, len(X_FAR))
    new_pairs = nt(rows16, wkv[...])
    flat = pairs.reshape(KV * 2, 128)
    gates = jnp.zeros((B, 128), F32)
    for k, piece in enumerate(split3(f_part)):
        gates = jnp.where(lane == k, piece, gates)
    for h in range(2):
        flat[pl.ds(2 * h, B, stride=4), :] = new_pairs
        flat[pl.ds(2 * h + 1, B, stride=4), :] = gates
    m2[...] = pairs[...].astype(BF16)
    b2[kv] = m2[kv]
    rk, ra = both(KV_FAR, kv_peer, ((lambda a: m2.at[a], b2), (lambda a: qa.at[kv], qa)), kv)
    rb = spread(KV_FAR, kv_peer, qb, kv)

    l_wg.wait()
    l_wu.wait()
    row16 = iota((B, 128), 0)
    gh, gmid, gl = split3(gain1)
    gain_rows = jnp.where(
        row16 == 0, gh, jnp.where(row16 == 1, gmid, jnp.where(row16 == 2, gl, 0.0))
    ).astype(BF16)
    gbuf[0:1, 0:UNITS] = jnp.sum(nt(gain_rows, wg[...]), axis=0, keepdims=True)
    gbuf[1:2, 0:UNITS] = jnp.sum(nt(gain_rows, wu[...]), axis=0, keepdims=True)
    for h in range(2):
        for t in range(3):
            at = (h * 3 + t) * 128
            gtile[h, t : t + 1, :] = gbuf[0:1, at : at + 128]
            gtile[h, 3 + t : 4 + t, :] = gbuf[1:2, at : at + 128]
    gm[...] = gtile[...].astype(BF16)
    bg[kv] = gm[lax.rem(kv, 2)]
    l_gs.wait()
    l_kv.wait()
    l_len.wait()
    l_bias.wait()

    first = iota((8, POS), 0) < 4
    first128 = iota((8, 128), 0) < 4
    position = iota((8, POS), 1) + kv * POS
    low8 = iota((8, 128), 1) < DH
    row32 = iota((32, 128), 0)
    lane32 = iota((32, 128), 1)

    own_pair = []

    def attend(half, buf):
        base = 32 * half
        rows32 = pl.ds(base, 32)
        summed = jnp.sum(buf[...].astype(F32), axis=0).astype(BF16).astype(F32) * scale
        tiles = (summed[0:8], summed[8:16])
        for j in range(4):
            t = tiles[j // 2]
            t = pltpu.roll(t, DH, 1) if j % 2 else t
            qs[pl.ds(base + j, 8, stride=4), :] = jnp.where(low8, t, 0.0)
        for p in range(4 * half, 4 * half + 4):
            own = pl.ds(8 * p, 8)
            queries = qs[own, :].astype(BF16)
            s = jnp.where(first, nt(queries, cache[2 * p]), nt(queries, cache[2 * p + 1]))
            s = s + jnp.where(first, gs[2 * p], gs[2 * p + 1])
            live = position < jnp.where(first, lengths[2 * p], lengths[2 * p + 1])
            scores[own, :] = jnp.where(live, s, EMPTY_SCORE)
        if not own_pair:
            rk.wait()
            own_pair.append(jnp.sum(b2[...].astype(F32), axis=0))
        pair = own_pair[0][0:1, :].astype(BF16).astype(F32)
        own_value = pair
        gate_in = lane_sum(own_pair[0][1:2, :], 0, 3) + bias[tp]
        new_gate = jnp.minimum(gate_in, 0.0) - jnp.log1p(jnp.exp(-jnp.abs(gate_in)))
        own_score = jnp.sum(qs[rows32, :] * pair, axis=1, keepdims=True) - new_gate
        here = (row32[:, 0:1] // 2) == kv - 16 * half
        own_score = jnp.where(here, own_score, EMPTY_SCORE)
        s = scores[rows32, :]
        top = jnp.maximum(jnp.max(s, axis=1, keepdims=True), own_score)
        own_weight = jnp.where(here, jnp.exp(own_score - top), 0.0)
        w = jnp.where(s > 0.5 * EMPTY_SCORE, jnp.exp(s - top), 0.0)
        total = jnp.sum(w, axis=1, keepdims=True) + own_weight
        weights[rows32, :] = w.astype(BF16)
        for p in range(4 * half, 4 * half + 4):
            own = pl.ds(8 * p, 8)
            w16 = weights[own, :]
            osum[own, :] = jnp.where(
                first128,
                jnp.dot(w16, cache[2 * p], preferred_element_type=F32),
                jnp.dot(w16, cache[2 * p + 1], preferred_element_type=F32),
            )
        osum[rows32, :] = osum[rows32, :] + own_weight.astype(BF16).astype(F32) * own_value
        o = [osum[pl.ds(base + j, 8, stride=4), :] for j in range(4)]
        sums = [jnp.where(low8, pltpu.roll(o[2 * i], DH, 1), o[2 * i + 1]) for i in range(2)]
        stat = jnp.where(lane32 == row32, top, jnp.where(lane32 == row32 + 32, total, 0.0))
        return jnp.concatenate(sums, axis=0), jnp.sum(stat, axis=0, keepdims=True)

    mask8 = lax.rem(iota((8, 128), 1), 32) // 4 == iota((8, 128), 0)
    source = iota((128, 256), 0)
    pick = lax.rem(source, 4) == iota((128, 256), 1) // DH
    pick = jnp.where(pick & (source < 96), 1.0, 0.0).astype(BF16)

    def combine(buf, stats):
        stat = stats[...].reshape(KV, 128)
        joint = jnp.max(stat, axis=0, keepdims=True)
        e = jnp.exp(stat - joint)
        total = jnp.sum(pltpu.roll(stat, 96, 1) * e, axis=0, keepdims=True)
        factors = jnp.concatenate([e, total], axis=0)
        hi, mid, low_part = split3(jnp.where(iota(factors.shape, 1) < 32, factors, 0.0))
        packed = hi + pltpu.roll(mid, 32, 1) + pltpu.roll(low_part, 64, 1)
        wide = [jnp.where(mask8, packed[i : i + 1, :], 0.0) for i in range(KV + 1)]
        wide = jnp.concatenate(wide, axis=0).astype(BF16)
        wide = jnp.dot(wide, pick, preferred_element_type=F32)
        acc = [0.0, 0.0]
        for i in range(KV):
            part = buf[i].astype(F32)
            for c in range(2):
                acc[c] = acc[c] + part[8 * c : 8 * c + 8] * wide[8 * i : 8 * i + 8, 128 * c : 128 * c + 128]
        return [acc[c] / wide[8 * KV :, 128 * c : 128 * c + 128] for c in range(2)]

    ra.wait()
    message, stat = attend(0, qa)
    aa[kv] = message.astype(BF16)
    tok_row = jnp.sum(jnp.where(lane == row16 + 64, t_part, 0.0), axis=0, keepdims=True)
    sa[kv] = stat + tok_row
    got_a = both(KV_FAR, kv_peer, ((lambda a: sa.at[kv], sa), (lambda a: aa.at[kv], aa)), kv)
    rb.wait()
    message, stat = attend(1, qb)
    ab[kv] = message.astype(BF16)
    sb[kv] = stat
    got_b = both(KV_FAR, kv_peer, ((lambda a: sb.at[kv], sb), (lambda a: ab.at[kv], ab)), kv)
    l_wo.wait()
    for r in got_a:
        r.wait()
    part_a = combine(aa, sa)
    tok_total = jnp.sum(sa[...].reshape(KV, 128), axis=0, keepdims=True)
    tok_mean = jnp.sum(jnp.where(lane == row16 + 64, tok_total, 0.0), axis=1, keepdims=True) * (1.0 / D)
    for r in got_b:
        r.wait()
    part_b = combine(ab, sb)
    attended = [jnp.concatenate([part_a[c], part_b[c]], axis=0).astype(BF16) for c in range(2)]

    proj = jnp.dot(attended[0], wo[0:128, :], preferred_element_type=F32)
    proj = proj + jnp.dot(attended[1], wo[128:256, :], preferred_element_type=F32)
    b4[tp] = proj.astype(BF16)
    r = spread(TP_FAR, tp_peer, b4, tp)
    rg = exchange(KV_FAR, kv_peer, lambda a: gm.at[lax.rem(a, 2)], bg, kv)
    r.wait()
    centred = rows + jnp.sum(b4[...].astype(F32), axis=0) - tok_mean

    gained_rows = (centred * gain1).astype(BF16)
    stat = small_tile(
        jnp.sum(centred, axis=1, keepdims=True), jnp.sum(centred * centred, axis=1, keepdims=True)
    )
    for h in range(2):
        sbuf[pl.ds(h * 8 + 6, B, stride=16), :] = stat
    for which, w in enumerate((wg, wu)):
        pbuf[which, :, 0:UNITS] = nt(gained_rows, w[...])
        for h in range(2):
            for t in range(3):
                at = (h * 3 + t) * 128
                sbuf[pl.ds(h * 8 + which * 3 + t, B, stride=16), :] = pbuf[which, :, at : at + 128]
    m5[...] = sbuf[...].reshape(KV, 8, 128).astype(BF16)
    b5[kv] = m5[kv]
    r = exchange(KV_FAR, kv_peer, lambda a: m5.at[a], b5, kv)
    rg.wait()
    gained = jnp.sum(bg[...].astype(F32), axis=0)
    r.wait()
    units = jnp.sum(b5[...].astype(F32), axis=0)
    lane_row = iota((1, 128), 1)
    srow = units[6:7, :]
    mean = lane_sum(srow, 0, 3) * (1.0 / D)
    spread1 = lane_sum(srow, 3, 6) * (1.0 / D) - mean * mean
    rstd = lax.rsqrt(spread1 + EPSILON)
    units = (units - mean * gained) * rstd
    gates = units[0:3, :]
    hidden = gates / (1.0 + jnp.exp(-gates)) * units[3:6, :]
    b6[kv, 0:3, :] = hidden
    b6[kv, 3:4, :] = jnp.where(lane_row == 0, mean, jnp.where(lane_row == 1, rstd, 0.0))
    r = spread(KV_FAR, kv_peer, b6, kv)
    l_wd.wait()
    r.wait()
    flat = b6.reshape(KV * 4, 128)
    tiles = [
        flat[pl.ds(h * 4 + t, B, stride=8), :].astype(BF16) for h in range(2) for t in range(3)
    ]
    norms = flat[pl.ds(3, B, stride=8), :]
    down = jnp.dot(jnp.concatenate(tiles, axis=1), wd[...], preferred_element_type=F32)

    b7[tp] = down.astype(BF16)
    r = spread(TP_FAR, tp_peer, b7, tp)
    mid = (centred - lane_sum(norms, 0, 1)) * lane_sum(norms, 1, 2) * gain1
    mid = mid.astype(BF16).astype(F32)
    r.wait()
    mixed = mid + jnp.sum(b7[...].astype(F32), axis=0)

    sum2 = jnp.sum(mixed, axis=1, keepdims=True)
    off = mixed - sum2 * (1.0 / 128)
    square2 = jnp.sum(off * off, axis=1, keepdims=True)
    stat = jnp.where(lane == row16, sum2, jnp.where(lane == row16 + B, square2, 0.0))
    b8[kv] = jnp.sum(stat, axis=0, keepdims=True)
    r = spread(KV_FAR, kv_peer, b8, kv)
    r.wait()
    stats = b8[...].reshape(KV, 128)
    total2 = jnp.sum(stats, axis=0, keepdims=True)
    drift = stats * (1.0 / 128) - total2 * (1.0 / D)
    between = jnp.sum(drift * drift, axis=0, keepdims=True) * 128.0
    mean2 = jnp.sum(jnp.where(lane == row16, total2, 0.0), axis=1, keepdims=True) * (1.0 / D)
    var2 = jnp.sum(
        jnp.where(lane == row16, between, jnp.where(lane == row16 + B, total2, 0.0)),
        axis=1, keepdims=True,
    ) * (1.0 / D)
    result = ((mixed - mean2) * lax.rsqrt(var2 + EPSILON) * gain2).astype(BF16)
    chosen = jnp.where(iota((8, 128), 1) == iota((8, 128), 0) + tp * 8, 1.0, 0.0).astype(BF16)
    out[...] = nt(chosen, result).astype(BF16)
    for w in waits:
        w.wait()


def on_device(
    tokens, live_lengths, kv_cache, gate_sums, w_query, w_key, w_value, w_forget, forget_bias,
    w_out, first_gain, w_gate, w_up, w_down, second_gain,
):
    hbm = pl.BlockSpec(memory_space=pl.ANY)
    vmem = pltpu.VMEM
    turned = pl.pallas_call(
        kernel,
        out_shape=pltpu.VMEM((8, B), BF16),
        in_specs=[hbm] * 15,
        out_specs=pl.BlockSpec(memory_space=pltpu.VMEM),
        scratch_shapes=[
            vmem((B, POS, 128), BF16),
            vmem((B, 1, POS), F32),
            vmem((128, 256), BF16),
            vmem((128, 128), BF16),
            vmem((16, 128), BF16),
            vmem((256, 128), BF16),
            vmem((UNITS, 128), BF16),
            vmem((UNITS, 128), BF16),
            vmem((WIDE, 128), BF16),
            vmem((8, B), BF16),
            vmem((2, 1, 8), F32),
            vmem((TP, 8, 128), F32),
            vmem((KV, B, 128), BF16),
            vmem((KV, B, 128), BF16),
            vmem((KV, 2, 128), F32),
            vmem((KV, 2, 128), BF16),
            vmem((KV, 2, 128), BF16),
            vmem((KV, B, 128), BF16),
            vmem((KV, B, 128), BF16),
            vmem((KV, 1, 128), F32),
            vmem((KV, 1, 128), F32),
            vmem((TP, B, 128), BF16),
            vmem((2, 8, 128), BF16),
            vmem((KV, 8, 128), BF16),
            vmem((KV, 8, 128), BF16),
            vmem((KV, 8, 128), BF16),
            vmem((KV, 4, 128), F32),
            vmem((TP, B, 128), BF16),
            vmem((KV, 1, 128), F32),
            vmem((64, 128), F32),
            vmem((64, 128), F32),
            vmem((64, POS), F32),
            vmem((64, POS), BF16),
            vmem((64, 128), F32),
            vmem((64, 128), F32),
            vmem((64, 128), F32),
            vmem((2, B, WIDE), F32),
            vmem((KV * 8, 128), F32),
            vmem((2, WIDE), F32),
            vmem((2, 8, 128), F32),
            pltpu.SMEM((B,), jnp.int32),
            pltpu.SMEM((TP,), F32),
            pltpu.SemaphoreType.REGULAR,
            pltpu.SemaphoreType.DMA((15,)),
            pltpu.SemaphoreType.DMA((14,)),
            pltpu.SemaphoreType.DMA((14,)),
        ],
        compiler_params=pltpu.CompilerParams(collective_id=0, has_side_effects=True),
    )(
        live_lengths, forget_bias, tokens.T, first_gain.reshape(1, 8), second_gain.reshape(1, 8),
        kv_cache, gate_sums, w_query, w_key.T, w_value.T, w_forget.T, w_out, w_gate.T, w_up.T,
        w_down,
    )
    return turned.T


def solution(mesh):
    placed = (
        P(None, ("kv", "tp")), P(), P(None, "kv", "tp"), P(None, "tp", "kv"), P("kv", "tp"),
        P("kv", "tp"), P("kv", "tp"), P(), P(), P("tp", "kv"), P(("kv", "tp")), P("kv", "tp"),
        P("kv", "tp"), P("tp", "kv"), P(("kv", "tp")),
    )
    return jax.shard_map(
        on_device, mesh=mesh, in_specs=placed, out_specs=P(None, ("kv", "tp")), check_vma=False
    )
```
